32 devices in a mesh: fs: 8 (over z, x), tp: 4 (over y, core).
Axes of the slice: x: 2, y: 2, z: 4, core: 2. Of those that a mesh axis runs over, the one named last changes fastest.
Arguments:
- later_rows: bfloat16 [3584, 2048], P(('fs', 'tp')), may hold values from -6 to 6
- earlier_rows: bfloat16 [3584, 2048], P(('fs', 'tp')), may hold values from -6 to 6
- cotangent: bfloat16 [3584, 2048], P(('fs', 'tp')), may hold values from -1 to 1
- gate_weight: bfloat16 [2048, 5632], P('fs', 'tp'), may hold values from -0.125 to 0.125
- up_weight: bfloat16 [2048, 5632], P('fs', 'tp'), may hold values from -0.125 to 0.125
- down_weight: bfloat16 [2048, 5632], P('fs', 'tp'), may hold values from -0.078125 to 0.078125
- gate_grad_sum: float32 [2048, 5632], P('fs', 'tp'), may hold values from -12 to 12
- up_grad_sum: float32 [2048, 5632], P('fs', 'tp'), may hold values from -12 to 12
- down_grad_sum: float32 [2048, 5632], P('fs', 'tp'), may hold values from -12 to 12
Outputs:
- later_out: bfloat16 [3584, 2048], P(('fs', 'tp'))
- input_grad: bfloat16 [3584, 2048], P(('fs', 'tp'))
- gate_grad_new: float32 [2048, 5632], P('fs', 'tp')
- up_grad_new: float32 [2048, 5632], P('fs', 'tp')
- down_grad_new: float32 [2048, 5632], P('fs', 'tp')
The draws below stay inside these ranges and needn't reach their ends.
All inputs are finite; a program needn't handle non-finite values.
Results may differ from the reference program's by a relative error of at most 0.014.
Values may be sent and summed in bfloat16 or wider, within the bound.
A program may use at most 128 MiB of HBM per device.

```python
import jax
import jax.numpy as jnp
from jax import lax

D = 2048
FF = 5632
TOKENS = 3584
N_TP = 4


def strengthened(values, stream_key, source, target, parts, factor):
    def block_of(position):
        return (jnp.arange(values.shape[position]) // (values.shape[position] // parts)).reshape((-1,) + (1,) * (values.ndim - 1 - position))

    first = jax.random.permutation(stream_key, parts)[block_of(target)]
    other_side = (block_of(target) + parts // 2) % parts
    return jnp.where((block_of(source) == first) | (block_of(source) == other_side), factor * values, values)


def block_scale(rng, shape, split, smallest, high):
    gain = 1.0
    for axis_at, shards_of in split:
        heights = jax.random.uniform(jax.random.fold_in(jax.random.fold_in(rng, 6), axis_at), (shards_of,), jnp.float32, smallest / len(split), high / len(split))
        gain = gain * jnp.repeat(jnp.exp(heights), shape[axis_at] // shards_of).reshape((-1,) + (1,) * (len(shape) - 1 - axis_at))
    return gain


def scatter_about(stream_key, shape, spread, limit, cuts=(), kind=jnp.bfloat16):
    drawn = jax.random.normal(stream_key, shape, jnp.float32) * spread
    if len(cuts) > 0:
        drawn = block_scale(stream_key, shape, cuts, -0.22, 0.18) * drawn
    return jnp.clip(drawn, min=-limit, max=limit).astype(kind)


def noise_with(rng, dims, spread, most, shards, heavy, held_as=jnp.bfloat16):
    drawn = spread * jax.random.normal(rng, dims, jnp.float32)
    if shards:
        drawn = drawn * block_scale(rng, dims, shards, -0.22, 0.18)
    return jnp.clip(strengthened(drawn, jax.random.fold_in(rng, 3), *heavy), -most, most).astype(held_as)


def setup_inputs(seed: int = 0) -> dict:
    streams_of = jax.random.split(jax.random.key(seed), 10)
    return {
        "later_rows": scatter_about(streams_of[0], (TOKENS, D), 1.0, 6.0, ((0, 32),)),
        "earlier_rows": scatter_about(streams_of[1], (TOKENS, D), 1.0, 6.0, ((0, 32),)),
        "cotangent": noise_with(streams_of[2], (TOKENS, D), 0.1, 1.0, ((0, 32),), (0, 1, 32, 2.75)),
        "gate_weight": scatter_about(streams_of[3], (D, FF), D ** -0.5, 0.125, ((0, 8), (1, 4))),
        "up_weight": scatter_about(streams_of[4], (D, FF), D ** -0.5, 0.125, ((0, 8), (1, 4))),
        "down_weight": scatter_about(streams_of[5], (D, FF), FF ** -0.5, 0.078125, ((0, 8), (1, 4))),
        "gate_grad_sum": scatter_about(streams_of[6], (D, FF), 2.0, 12.0, ((0, 8), (1, 4)), jnp.float32),
        "up_grad_sum": scatter_about(streams_of[7], (D, FF), 2.0, 12.0, ((0, 8), (1, 4)), jnp.float32),
        "down_grad_sum": scatter_about(streams_of[8], (D, FF), 2.0, 12.0, ((0, 8), (1, 4)), jnp.float32),
    }


def silu_parts(gate):
    sigma = jax.nn.sigmoid(gate)
    return gate * sigma, sigma * (1.0 + gate * (1.0 - sigma))


def by_columns(left, right):
    return lax.dot_general(left, right, (((1,), (1,)), ((), ())), preferred_element_type=jnp.float32)


def by_rows(left, right):
    return lax.dot_general(left, right, (((0,), (0,)), ((), ())), preferred_element_type=jnp.float32)


def reference(later_rows, earlier_rows, cotangent, gate_weight, up_weight, down_weight, gate_grad_sum, up_grad_sum, down_grad_sum):
    width = FF // N_TP
    later_gate = jnp.dot(later_rows, gate_weight, preferred_element_type=jnp.float32)
    later_up = jnp.dot(later_rows, up_weight, preferred_element_type=jnp.float32)
    later_hidden = (jax.nn.silu(later_gate) * later_up).astype(jnp.bfloat16)
    total = jnp.zeros((later_rows.shape[0], D), jnp.float32)
    for block in range(N_TP):
        lower = block * width
        part = by_columns(later_hidden[:, lower:lower + width], down_weight[:, lower:lower + width]).astype(jnp.bfloat16)
        total = total + lax.optimization_barrier(part).astype(jnp.float32)
    later_out = total.astype(jnp.bfloat16)

    gate_e = jnp.dot(earlier_rows, gate_weight, preferred_element_type=jnp.float32)
    up_e = jnp.dot(earlier_rows, up_weight, preferred_element_type=jnp.float32)
    activation, slope = silu_parts(gate_e)
    hidden_e = (activation * up_e).astype(jnp.bfloat16)
    back_hidden = jnp.dot(cotangent, down_weight, preferred_element_type=jnp.float32)
    gate_back = (back_hidden * up_e * slope).astype(jnp.bfloat16)
    up_back = (back_hidden * activation).astype(jnp.bfloat16)
    total = jnp.zeros((earlier_rows.shape[0], D), jnp.float32)
    for block in range(N_TP):
        lower = block * width
        part = by_columns(gate_back[:, lower:lower + width], gate_weight[:, lower:lower + width])
        part = part + by_columns(up_back[:, lower:lower + width], up_weight[:, lower:lower + width])
        total = total + lax.optimization_barrier(part.astype(jnp.bfloat16)).astype(jnp.float32)
    input_grad = total.astype(jnp.bfloat16)
    gate_grad_new = gate_grad_sum + by_rows(earlier_rows, gate_back)
    up_grad_new = up_grad_sum + by_rows(earlier_rows, up_back)
    down_grad_new = down_grad_sum + by_rows(cotangent, hidden_e)
    return later_out, input_grad, gate_grad_new, up_grad_new, down_grad_new
```

```python
import jax
import jax.numpy as jnp
from jax import lax
from jax.sharding import Mesh, PartitionSpec as P


def silu_parts(gate):
    sigma = jax.nn.sigmoid(gate)
    return (gate * sigma, sigma * (1.0 + gate * (1.0 - sigma)))


def by_columns(left, right):
    return lax.dot_general(
        left, right, (((1,), (1,)), ((), ())), preferred_element_type=jnp.float32
    )


def by_rows(left, right):
    return lax.dot_general(
        left, right, (((0,), (0,)), ((), ())), preferred_element_type=jnp.float32
    )


def dot(left, right):
    return jnp.dot(left, right, preferred_element_type=jnp.float32)


def pick(index, choices):
    value = choices[-1]
    for at in range(len(choices) - 2, -1, -1):
        value = jnp.where(index == at, choices[at], value)
    return value


def shift(value, axis, size, by):
    return lax.ppermute(value, axis, [(i, (i + by) % size) for i in range(size)])


def spread_columns(weight, nx):
    x = lax.axis_index("x")
    rows, columns = weight.shape[0], weight.shape[1] // nx
    parts = [weight[:, c * columns : (c + 1) * columns] for c in range(nx)]
    whole = [pick(x, parts)]
    for by in range(1, nx):
        whole.append(shift(pick((x + by) % nx, parts), "x", nx, by))
    return jnp.concatenate([pick((x - c) % nx, whole) for c in range(nx)], axis=0)


def join_columns(total, nx):
    x = lax.axis_index("x")
    rows = total.shape[0] // nx
    parts = [total[c * rows : (c + 1) * rows] for c in range(nx)]
    whole = [pick(x, parts)]
    for by in range(1, nx):
        sent = pick((x + by) % nx, parts).astype(jnp.bfloat16)
        whole.append(shift(sent, "x", nx, by).astype(jnp.float32))
    return jnp.concatenate([pick((x - c) % nx, whole) for c in range(nx)], axis=1)


def gather_line(block, nz):
    z = lax.axis_index("z")
    up = down = block
    ups, downs = [block], [block]
    for step in range(1, nz):
        up = lax.ppermute(up, "z", [(i, i + 1) for i in range(step - 1, nz - 1)])
        down = lax.ppermute(down, "z", [(i, i - 1) for i in range(1, nz - step + 1)])
        ups.append(up)
        downs.append(down)
    rows = block.shape[0]
    whole = jnp.zeros((nz * rows, block.shape[1]), block.dtype)
    whole = lax.dynamic_update_slice_in_dim(whole, block, z * rows, 0)
    for back in range(1, nz):
        arrived = jnp.where(z >= back, ups[back], downs[nz - back])
        whole = lax.dynamic_update_slice_in_dim(whole, arrived, ((z - back) % nz) * rows, 0)
    return whole


def scatter_line(parts, nz):
    z = lax.axis_index("z")
    rows = parts.shape[0] // nz

    def block(index):
        return lax.dynamic_slice_in_dim(parts, (index % nz) * rows, rows, 0)

    up = down = None
    for step in range(1, nz):
        up_sum, down_sum = block(z - step), block(z + step)
        if step > 1:
            up_sum = up_sum + up.astype(jnp.float32)
            down_sum = down_sum + down.astype(jnp.float32)
        up = lax.ppermute(
            up_sum.astype(jnp.bfloat16), "z", [(i, i + 1) for i in range(min(step, nz - 1))]
        )
        down = lax.ppermute(
            down_sum.astype(jnp.bfloat16), "z", [(i, i - 1) for i in range(max(nz - step, 1), nz)]
        )
    total = block(z)
    if nz > 1:
        total = total + up.astype(jnp.float32) + down.astype(jnp.float32)
    return total


def solution(mesh):
    nf, nt = mesh.shape["fs"], mesh.shape["tp"]
    nx = max(d for d in range(1, nf + 1) if nf % d == 0 and d * d <= nf)
    nz = nf // nx
    split = Mesh(mesh.devices.reshape(nz, nx, nt), ("z", "x", "tp"))
    plane = ("x", "tp")

    def local(
        later_rows,
        earlier_rows,
        cotangent,
        gate_weight,
        up_weight,
        down_weight,
        gate_grad_sum,
        up_grad_sum,
        down_grad_sum,
    ):
        gate_full = gather_line(spread_columns(gate_weight, nx), nz)
        up_full = gather_line(spread_columns(up_weight, nx), nz)
        down_full = gather_line(spread_columns(down_weight, nx), nz)
        rows_all = lax.all_gather(earlier_rows, plane, axis=0, tiled=True)
        back_all = lax.all_gather(cotangent, plane, axis=0, tiled=True)
        piece = lax.all_gather(later_rows, plane, axis=0, tiled=True)

        gate_e = dot(rows_all, gate_full)
        up_e = dot(rows_all, up_full)
        activation, act_slope = silu_parts(gate_e)
        hidden_e = (activation * up_e).astype(jnp.bfloat16)
        down_grad = scatter_line(by_rows(back_all, hidden_e), nz)
        back_hidden = dot(back_all, down_full)
        gate_back = (back_hidden * up_e * act_slope).astype(jnp.bfloat16)
        up_back = (back_hidden * activation).astype(jnp.bfloat16)
        gate_grad = scatter_line(by_rows(rows_all, gate_back), nz)
        up_grad = scatter_line(by_rows(rows_all, up_back), nz)
        input_grad = lax.psum_scatter(
            (by_columns(gate_back, gate_full) + by_columns(up_back, up_full)).astype(jnp.bfloat16),
            plane,
            scatter_dimension=0,
            tiled=True,
        )
        later_hidden = (jax.nn.silu(dot(piece, gate_full)) * dot(piece, up_full)).astype(jnp.bfloat16)
        later_out = lax.psum_scatter(
            by_columns(later_hidden, down_full).astype(jnp.bfloat16),
            plane,
            scatter_dimension=0,
            tiled=True,
        )
        return (
            later_out,
            input_grad,
            gate_grad_sum + join_columns(gate_grad, nx),
            up_grad_sum + join_columns(up_grad, nx),
            down_grad_sum + join_columns(down_grad, nx),
        )

    rows, weights = P(("z", "x", "tp"), None), P(("z", "x"), "tp")
    return jax.shard_map(
        local,
        mesh=split,
        in_specs=(rows,) * 3 + (weights,) * 6,
        out_specs=(rows,) * 2 + (weights,) * 3,
        check_vma=False,
    )
```

```python
import jax
import jax.numpy as jnp
from jax import lax
from jax.sharding import Mesh, PartitionSpec as P


def silu_parts(gate):
    sigma = jax.nn.sigmoid(gate)
    return (gate * sigma, sigma * (1.0 + gate * (1.0 - sigma)))


def by_columns(left, right):
    return lax.dot_general(
        left, right, (((1,), (1,)), ((), ())), preferred_element_type=jnp.float32
    )


def by_rows(left, right):
    return lax.dot_general(
        left, right, (((0,), (0,)), ((), ())), preferred_element_type=jnp.float32
    )


def dot(left, right):
    return jnp.dot(left, right, preferred_element_type=jnp.float32)


def pick(index, choices):
    value = choices[-1]
    for at in range(len(choices) - 2, -1, -1):
        value = jnp.where(index == at, choices[at], value)
    return value


def shift(value, axis, size, by):
    return lax.ppermute(value, axis, [(i, (i + by) % size) for i in range(size)])


def spread_columns(weight, nx):
    x = lax.axis_index("x")
    rows, columns = weight.shape[0], weight.shape[1] // nx
    parts = [weight[:, c * columns : (c + 1) * columns] for c in range(nx)]
    whole = [pick(x, parts)]
    for by in range(1, nx):
        whole.append(shift(pick((x + by) % nx, parts), "x", nx, by))
    return jnp.concatenate([pick((x - c) % nx, whole) for c in range(nx)], axis=0)


def join_columns(total, nx):
    x = lax.axis_index("x")
    rows = total.shape[0] // nx
    parts = [total[c * rows : (c + 1) * rows] for c in range(nx)]
    whole = [pick(x, parts)]
    for by in range(1, nx):
        sent = pick((x + by) % nx, parts).astype(jnp.bfloat16)
        whole.append(shift(sent, "x", nx, by).astype(jnp.float32))
    return jnp.concatenate([pick((x - c) % nx, whole) for c in range(nx)], axis=1)


def after(value, *earlier):
    return lax.optimization_barrier((value,) + earlier)[0]


def gather_line(block, nz, middle=lambda: ((), ())):
    z = lax.axis_index("z")
    ahead_step, ahead_use = middle()
    up = down = block
    ups, downs = [block], [block]
    for step in range(1, nz):
        if step == nz - 1 and ahead_step:
            up, down = after(up, *ahead_step), after(down, *ahead_step)
        up = lax.ppermute(up, "z", [(i, i + 1) for i in range(step - 1, nz - 1)])
        down = lax.ppermute(down, "z", [(i, i - 1) for i in range(1, nz - step + 1)])
        ups.append(up)
        downs.append(down)
    rows = block.shape[0]
    whole = jnp.zeros((nz * rows, block.shape[1]), block.dtype)
    whole = lax.dynamic_update_slice_in_dim(whole, block, z * rows, 0)
    for back in range(1, nz):
        arrived = jnp.where(z >= back, ups[back], downs[nz - back])
        if ahead_use:
            arrived = after(arrived, *ahead_use)
        whole = lax.dynamic_update_slice_in_dim(whole, arrived, ((z - back) % nz) * rows, 0)
    return whole, (ups[max(nz - 2, 0)], downs[max(nz - 2, 0)])


def scatter_line(parts, nz):
    z = lax.axis_index("z")
    rows = parts.shape[0] // nz

    def block(index):
        return lax.dynamic_slice_in_dim(parts, (index % nz) * rows, rows, 0)

    up = down = None
    first = ()
    for step in range(1, nz):
        up_sum, down_sum = block(z - step), block(z + step)
        if step > 1:
            up_sum = up_sum + up.astype(jnp.float32)
            down_sum = down_sum + down.astype(jnp.float32)
        up = lax.ppermute(
            up_sum.astype(jnp.bfloat16), "z", [(i, i + 1) for i in range(min(step, nz - 1))]
        )
        down = lax.ppermute(
            down_sum.astype(jnp.bfloat16), "z", [(i, i - 1) for i in range(max(nz - step, 1), nz)]
        )
        first = first or (up, down)
    total = block(z)
    if nz > 1:
        total = total + up.astype(jnp.float32) + down.astype(jnp.float32)
    return total, first


def solution(mesh):
    nf, nt = mesh.shape["fs"], mesh.shape["tp"]
    nx = max(d for d in range(1, nf + 1) if nf % d == 0 and d * d <= nf)
    nz = nf // nx
    split = Mesh(mesh.devices.reshape(nz, nx, nt), ("z", "x", "tp"))
    plane = ("x", "tp")

    def local(
        later_rows,
        earlier_rows,
        cotangent,
        gate_weight,
        up_weight,
        down_weight,
        gate_grad_sum,
        up_grad_sum,
        down_grad_sum,
    ):
        gate_full, gate_last = gather_line(spread_columns(gate_weight, nx), nz)
        up_full, up_last = gather_line(spread_columns(up_weight, nx), nz)
        rows_all = lax.all_gather(earlier_rows, plane, axis=0, tiled=True)
        back_all = lax.all_gather(cotangent, plane, axis=0, tiled=True)
        piece = lax.all_gather(after(later_rows, *gate_last), plane, axis=0, tiled=True)

        gate_e = dot(rows_all, gate_full)
        up_e = dot(rows_all, up_full)
        activation, act_slope = silu_parts(gate_e)
        hidden_e = (activation * up_e).astype(jnp.bfloat16)
        down_parts = by_rows(back_all, hidden_e)
        down_grad, down_first = scatter_line(down_parts, nz)
        later_hidden = (jax.nn.silu(dot(piece, gate_full)) * dot(piece, up_full)).astype(jnp.bfloat16)
        down_block = after(spread_columns(down_weight, nx), *gate_last, *up_last)
        down_full, _ = gather_line(down_block, nz, lambda: ((gate_e, up_e), (down_parts, later_hidden) + down_first))
        later_parts = by_columns(later_hidden, down_full).astype(jnp.bfloat16)
        later_out = lax.psum_scatter(later_parts, plane, scatter_dimension=0, tiled=True)
        back_hidden = dot(back_all, down_full)
        gate_back = (back_hidden * up_e * act_slope).astype(jnp.bfloat16)
        up_back = (back_hidden * activation).astype(jnp.bfloat16)
        gate_parts = by_rows(rows_all, gate_back)
        up_parts = by_rows(rows_all, up_back)
        gate_grad, gate_first = scatter_line(gate_parts, nz)
        up_grad, _ = scatter_line(up_parts, nz)
        gate_back = after(gate_back, *gate_first)
        up_back = after(up_back, *gate_first)
        input_grad = lax.psum_scatter(
            after(
                (by_columns(gate_back, gate_full) + by_columns(up_back, up_full)).astype(jnp.bfloat16),
                later_out,
            ),
            plane,
            scatter_dimension=0,
            tiled=True,
        )
        return (
            later_out,
            input_grad,
            gate_grad_sum + join_columns(gate_grad, nx),
            up_grad_sum + join_columns(up_grad, nx),
            down_grad_sum + join_columns(down_grad, nx),
        )

    rows, weights = P(("z", "x", "tp"), None), P(("z", "x"), "tp")
    return jax.shard_map(
        local,
        mesh=split,
        in_specs=(rows,) * 3 + (weights,) * 6,
        out_specs=(rows,) * 2 + (weights,) * 3,
        check_vma=False,
    )
```
